32 devices in a mesh: grp: 2 (over y), ep: 16 (over z, x, core), tp: 1.
Axes of the slice: x: 2, y: 2, z: 4, core: 2. Of those that a mesh axis runs over, the one named last changes fastest.
Arguments:
- tokens: bfloat16 [2048, 2048], P(('grp', 'ep')), parts along dimension 0, may hold values from -6 to 6
- norm_gain: float32 [2048], replicated, may hold values from 0.1 to 1.9
- routes: int32 [2048, 6], P(('grp', 'ep')), parts along dimension 0, may hold values from 0 to 15, all different within a row; in each aligned block of 64 rows (0 to 63, 64 to 127, ...) at most 48 rows name the same one
- route_weights: float32 [2048, 6], P(('grp', 'ep')), parts along dimension 0, may hold values from 0.05 to 1
- w_gate: bfloat16 [16, 2048, 2048], P('ep', None, 'tp'), may hold values from -0.125 to 0.125
- w_up: bfloat16 [16, 2048, 2048], P('ep', None, 'tp'), may hold values from -0.125 to 0.125
- w_down: bfloat16 [16, 2048, 2048], P('ep', 'tp'), may hold values from -4 to 4
- final_gain: float32 [2048], P('tp'), may hold values from 0.1 to 1.9
Outputs:
- mixed_out: bfloat16 [2048, 2048], P(('grp', 'ep'), 'tp'), parts along dimension 0
The draws below stay inside these ranges and needn't reach their ends.
There are 2 independent parts, one for each index of `grp`. The reference program is written for one: setup_inputs(seed, part) draws one part's arguments, and reference() takes and returns one part's arrays. A program takes and returns all parts, laid end to end along the dimension named above; an argument that names none is the same for every part. Nothing has to cross between parts.
Inputs may be any that keep to these rules, and one draw needn't show every extreme that they name: `routes`: each row names 6 different experts; within the rows of one index of ep no expert is named by more than 48 rows, and in every draw some expert is named by exactly 48 rows of some index.
All inputs are finite; a program needn't handle non-finite values.
Results may differ from the reference program's by a relative error of at most 0.015.
Values may be sent and summed in bfloat16 or wider, within the bound.
No kernel may reach another device: no remote copies, remote signals or barrier semaphores. Data moves between devices by JAX's collectives and lax.ppermute only.
A program may use at most 64 MiB of HBM per device.

```python
import math
import jax
import jax.numpy as jnp
import numpy as np
from jax import lax

D = 2048
FF = 2048
TOP_K = 6
TOK_DEV = 64
EXPERTS = 16
CAP = 48
TOKENS = 1024
N_EP = 16
N_TP = 1


def draw_w_down(key, part):
    key_values, key_columns = jax.random.split(key)
    columns = jnp.arange(D, dtype=jnp.float32) / D
    roughness = jax.random.uniform(key_columns, (D,), jnp.float32, 0.5, 1.5)
    values = jnp.clip(jax.random.normal(key_values, (EXPERTS, FF, D), jnp.float32), -5.0, 5.0)
    column_scale = jnp.exp(columns * jnp.log(10.0)) * roughness
    scaled = values * column_scale[None, None, :] * FF ** (-0.5) / 3.0
    return scaled.astype(jnp.bfloat16)


def block_scale(own_key, shape, cuts, smallest, high):
    loudness, own = 1.0, jax.random.fold_in(own_key, 6)
    for position, blocks in cuts:
        steps = jnp.exp(jax.random.uniform(jax.random.fold_in(own, position), (blocks,), jnp.float32, smallest / len(cuts), high / len(cuts)))
        loudness = loudness * jnp.repeat(steps, shape[position] // blocks).reshape([-1 if axis == position else 1 for axis in range(len(shape))])
    return loudness


def deal_out(key, own, number, rows, count, top, reach, slope):
    order = jax.random.permutation(key, count)
    crowded, common = load_shares(count, rows * top, reach, slope, True), load_shares(count, rows * top, reach, slope, False)
    places = jnp.arange(count)

    def named(sizes, offset_by):
        used = int((sizes > 0).sum())
        fixed = max(1, used // 4)
        shifted = fixed + (places - fixed + offset_by * (used - fixed)) % max(1, count - fixed)
        return jnp.zeros((count,), jnp.int32).at[order[jnp.where(places < fixed, places, shifted)]].set(jnp.asarray(sizes, jnp.int32))

    sizes = jnp.where(number % 4 == 0, named(crowded, number // 4), named(common, number - number // 4 - 1))
    mixed = jax.random.permutation(jax.random.fold_in(own, 3), count)
    source_of, taker = mixed[0:count // 2 * 2:2], mixed[1:count // 2 * 2:2]
    margin = jnp.minimum(sizes[source_of] - 1, reach - sizes[taker]) // 2
    margin = jnp.where((source_of == order[0]) | (taker == order[0]) | (sizes[taker] == 0), 0, jnp.maximum(margin, 0))
    shifted = jax.random.randint(jax.random.fold_in(own, 4), (count // 2,), 0, 1 << 20) % (margin + 1)
    sizes = sizes.at[source_of].add(-shifted).at[taker].add(shifted)
    labels = jnp.searchsorted(jnp.cumsum(sizes), jnp.arange(rows * top), side="right").astype(jnp.int32)
    listing = labels.reshape(top, rows).T
    listing = listing[jax.random.permutation(jax.random.fold_in(own, 1), rows)]
    offset_by = jax.random.randint(jax.random.fold_in(own, 2), (rows, 1), 0, top)
    return jnp.take_along_axis(listing, (jnp.arange(top)[None, :] + offset_by) % top, axis=1)


def load_shares(number_of, total, reach, slope, full):
    weights = [(1 << 20) // math.isqrt(standing ** slope) + 1 for standing in range(1, number_of + 1)]
    largest = reach if full else min(reach, max(-(-total // number_of), total * weights[0] // sum(weights)))
    least = 1 if total - largest >= number_of - 1 else 0
    counts, surplus = [largest] + [least] * (number_of - 1), total - largest - least * (number_of - 1)
    while surplus > 0:
        candidates = [i for i in range(1, number_of) if counts[i] < largest] or [i for i in range(1, number_of) if counts[i] < reach]
        mass, left = sum([weights[i] for i in candidates]), surplus
        for i in candidates:
            more = min(reach - counts[i], max(1, left * weights[i] // mass), surplus)
            counts[i] = counts[i] + more
            surplus = surplus - more
    return np.array(counts)


def scatter_about(rng, shape, deviation, bound, cuts=(), kind=jnp.bfloat16):
    loudness = block_scale(rng, shape, cuts, -0.22, 0.18) if cuts else 1.0
    array = jax.random.normal(rng, shape, jnp.float32) * deviation * loudness
    return jnp.minimum(jnp.maximum(array, -bound), bound).astype(kind)


def setup_inputs(seed: int = 0, part: int = 0) -> dict:
    keys = jax.random.split(jax.random.key(seed), 9)
    part_splits = jax.random.split(jax.random.fold_in(keys[8], part), 9)
    tokens = scatter_about(part_splits[0], (TOKENS, D), 1.0, 6.0, ((0, 16),))
    norm_gain = jnp.clip(1.0 + 0.18 * jax.random.normal(keys[1], (D,), jnp.float32), 0.1, 1.9)
    routes_keys = jax.random.split(jax.random.fold_in(part_splits[2], 1), TOKENS // TOK_DEV)
    routes_turns = jax.random.permutation(jax.random.fold_in(part_splits[2], 3), TOKENS // TOK_DEV)
    routes = jax.vmap(lambda own, number: deal_out(jax.random.fold_in(part_splits[2], 2), own, number, TOK_DEV, EXPERTS, TOP_K, CAP, 2))(routes_keys, routes_turns).reshape((TOKENS, TOP_K))
    route_weights = jnp.clip(jnp.exp(math.log(1.0) - 2.9957323 * jax.random.uniform(part_splits[3], (TOKENS, TOP_K), jnp.float32) ** block_scale(part_splits[3], (TOKENS, TOP_K), ((0, 16),), -0.2, 0.2)), 0.05, 1.0)
    w_gate = scatter_about(keys[4], (EXPERTS, D, FF), D ** -0.5, 0.125, ((0, 16),))
    w_up = scatter_about(keys[5], (EXPERTS, D, FF), D ** -0.5, 0.125, ((0, 16),))
    w_down = draw_w_down(jax.random.fold_in(keys[8], 71), part)
    final_gain = jnp.clip(1.0 + 0.18 * jax.random.normal(keys[7], (D,), jnp.float32), 0.1, 1.9)
    return dict(tokens=tokens, norm_gain=norm_gain, routes=routes, route_weights=route_weights, w_gate=w_gate, w_up=w_up, w_down=w_down, final_gain=final_gain)


EPS = 1e-06

def slot_table(route_rows):
    flattened = route_rows.reshape(-1)
    matches = (flattened[:, None] == jnp.arange(EXPERTS, dtype=jnp.int32)[None, :]).astype(jnp.int32)
    earlier = jnp.cumsum(matches, axis=0) - matches
    slot_of = lax.optimization_barrier(jnp.sum(earlier * matches, axis=1))
    return (flattened * CAP + slot_of).reshape(route_rows.shape).astype(jnp.int32)

def dispatch(place_block, row_block):
    slot_ids = jnp.arange(EXPERTS * CAP, dtype=jnp.int32)
    selector = lax.optimization_barrier(jnp.sum((place_block[None, :, :] == slot_ids[:, None, None]).astype(jnp.float32), axis=2))
    return jnp.dot(selector.astype(jnp.bfloat16), row_block, preferred_element_type=jnp.float32).astype(jnp.bfloat16)

def expert(inputs):
    row_block, gate_w, up_w, down_w = inputs
    gate_value = jnp.dot(row_block, gate_w, preferred_element_type=jnp.float32)
    up_value = jnp.dot(row_block, up_w, preferred_element_type=jnp.float32)
    hidden = (jax.nn.silu(gate_value) * up_value).astype(jnp.bfloat16)
    hidden_split = hidden.reshape(row_block.shape[0], N_TP, FF // N_TP).astype(jnp.float32)
    down_split = down_w.reshape(N_TP, FF // N_TP, D).astype(jnp.float32)
    partial_value = jnp.einsum('rjf,jfd->jrd', hidden_split, down_split).astype(jnp.bfloat16)
    partial_value = lax.optimization_barrier(partial_value)
    return lax.optimization_barrier(jnp.sum(partial_value.astype(jnp.float32), axis=0)).astype(jnp.bfloat16)

def reference(tokens, norm_gain, routes, route_weights, w_gate, w_up, w_down, final_gain):
    tokens_f = tokens.astype(jnp.float32)
    inverse = lax.rsqrt(lax.optimization_barrier(jnp.mean(tokens_f * tokens_f, axis=1, keepdims=True)) + EPS)
    normed = (tokens_f * inverse * norm_gain[None, :]).astype(jnp.bfloat16)
    blocks = normed.reshape(N_EP, TOK_DEV, D)
    places = jax.vmap(slot_table)(routes.reshape(N_EP, TOK_DEV, TOP_K))
    buffers = jax.vmap(dispatch)(places, blocks)
    expert_in = buffers.reshape(N_EP, EXPERTS, CAP, D).transpose(1, 0, 2, 3).reshape(EXPERTS, N_EP * CAP, D)
    expert_out = lax.map(expert, (expert_in, w_gate, w_up, w_down))
    by_block = expert_out.reshape(EXPERTS, N_EP, CAP, D).transpose(1, 0, 2, 3).reshape(N_EP, EXPERTS * CAP, D)
    block_ids = jnp.arange(N_EP, dtype=jnp.int32)[:, None, None]
    picked = by_block[block_ids, places].astype(jnp.float32)
    weights = route_weights.reshape(N_EP, TOK_DEV, TOP_K)
    combined = lax.optimization_barrier(jnp.sum(weights[:, :, :, None] * picked, axis=2)).reshape(TOKENS, D)
    inverse_out = lax.rsqrt(lax.optimization_barrier(jnp.mean(combined * combined, axis=1, keepdims=True)) + EPS)
    return (combined * inverse_out * final_gain[None, :]).astype(jnp.bfloat16)
```

```python
import jax
import jax.numpy as jnp
from jax import lax
from jax.sharding import PartitionSpec as P

TOP_K = 6
EPS = 1e-06
LANES = 128


def per_device(tokens, norm_gain, routes, route_weights, w_gate, w_up, w_down, final_gain):
    tok_count, features = tokens.shape
    ep_size = lax.axis_size("ep")
    exp_local = w_gate.shape[0]
    experts_all = exp_local * ep_size
    capacity = max(2, min(tok_count, 2 * tok_count * TOP_K // experts_all))
    tokens_f = tokens.astype(jnp.float32)
    inverse = lax.rsqrt(jnp.mean(tokens_f * tokens_f, axis=1, keepdims=True) + EPS)
    normed = (tokens_f * inverse * norm_gain[None, :]).astype(jnp.bfloat16)
    chosen = routes[:, :, None] == jnp.arange(experts_all, dtype=jnp.int32)[None, None, :]
    table = jnp.sum(jnp.where(chosen, route_weights[:, :, None], 0.0), axis=1)
    high = lax.reduce_precision(table, 8, 7)
    low = table - high
    side = jnp.concatenate([high, low], axis=1).astype(jnp.bfloat16)
    pad = -side.shape[1] % LANES
    side = jnp.pad(side, ((0, 0), (0, pad)))
    gathered = lax.all_gather(
        jnp.concatenate([normed, side], axis=1), "ep", axis=0, tiled=False
    )
    rows_all = gathered[:, :, :features]
    side_all = gathered[:, :, features:]
    base = lax.axis_index("ep") * exp_local
    total = jnp.zeros((ep_size, tok_count, features), jnp.float32)
    for e in range(exp_local):
        lanes = jnp.arange(side_all.shape[2], dtype=jnp.int32)
        mine = (lanes == base + e) | (lanes == experts_all + base + e)
        weight = jnp.sum(jnp.where(mine, side_all.astype(jnp.float32), 0.0), axis=2)
        used = weight > 0
        used_f = used.astype(jnp.float32)
        before = jnp.arange(tok_count)[:, None] < jnp.arange(tok_count)[None, :]
        place = jnp.dot(used_f, before.astype(jnp.float32))
        place = jnp.where(used, place.astype(jnp.int32), -1)
        slots = jnp.arange(capacity, dtype=jnp.int32)
        select = (place[:, None, :] == slots[None, :, None]).astype(jnp.bfloat16)
        slot_weight = jnp.sum(select.astype(jnp.float32) * weight[:, None, :], axis=2)
        rows = jnp.einsum("bst,btd->bsd", select, rows_all, preferred_element_type=jnp.float32)
        rows = rows.astype(jnp.bfloat16).reshape(ep_size * capacity, features)
        gate_value = jnp.dot(rows, w_gate[e], preferred_element_type=jnp.float32)
        up_value = jnp.dot(rows, w_up[e], preferred_element_type=jnp.float32)
        hidden = (jax.nn.silu(gate_value) * up_value).astype(jnp.bfloat16)
        value = jnp.dot(hidden, w_down[e], preferred_element_type=jnp.float32)
        value = value * slot_weight.reshape(-1, 1)
        value = value.astype(jnp.bfloat16).reshape(ep_size, capacity, features)
        total = total + jnp.einsum("bst,bsd->btd", select, value, preferred_element_type=jnp.float32)
    total = total.astype(jnp.bfloat16).reshape(ep_size * tok_count, features)
    total = lax.psum_scatter(total, "tp", scatter_dimension=1, tiled=True)
    combined = lax.psum_scatter(total, "ep", scatter_dimension=0, tiled=True).astype(jnp.float32)
    squares_all = lax.psum(jnp.sum(combined * combined, axis=1), "tp")
    inverse_out = lax.rsqrt(squares_all / features + EPS)
    return (combined * inverse_out[:, None] * final_gain[None, :]).astype(jnp.bfloat16)


def solution(mesh):
    placed = (
        P(("grp", "ep"), None),
        P(),
        P(("grp", "ep"), None),
        P(("grp", "ep"), None),
        P("ep", None, "tp"),
        P("ep", None, "tp"),
        P("ep", "tp", None),
        P("tp"),
    )
    return jax.shard_map(
        per_device, mesh=mesh, in_specs=placed, out_specs=P(("grp", "ep"), "tp"), check_vma=False
    )
```

```python
import functools

import jax
import jax.numpy as jnp
from jax import lax
from jax.experimental import pallas as pl
from jax.experimental.pallas import tpu as pltpu
from jax.sharding import PartitionSpec as P

TOP_K = 6
EPS = 1e-06
LANES = 128
FF_TILE = 512


def expert_kernel(*refs, blocks, features, capacity, steps):
    mask_ref, *refs = refs
    pieces, refs = refs[:blocks], refs[blocks:]
    gate_ref, up_ref, down_ref, *refs = refs
    outs, refs = refs[:blocks], refs[blocks:]
    rows_ref, acc_ref, pick_ref, weight_ref = refs
    step = pl.program_id(0)
    tok = pieces[0].shape[0]

    @pl.when(step == 0)
    def _():
        for b in range(blocks):
            side = pieces[b][:, features:].astype(jnp.float32)
            weight = jnp.sum(side * mask_ref[0:1, :], axis=1, keepdims=True)
            used = weight > 0
            later = lax.broadcasted_iota(jnp.int32, (tok, tok), 0)
            earlier = lax.broadcasted_iota(jnp.int32, (tok, tok), 1)
            below = (earlier < later).astype(jnp.bfloat16)
            flags = jnp.broadcast_to(used.astype(jnp.float32), (tok, LANES)).astype(jnp.bfloat16)
            place = jnp.dot(below, flags, preferred_element_type=jnp.float32)[:, :capacity]
            slots = lax.broadcasted_iota(jnp.int32, (tok, capacity), 1).astype(jnp.float32)
            pick = ((place == slots) & used).astype(jnp.bfloat16)
            pick_ref[b] = pick
            weight_ref[b] = weight
            rows = lax.dot_general(
                pick,
                pieces[b][:, :features],
                (((0,), (0,)), ((), ())),
                preferred_element_type=jnp.float32,
            )
            rows_ref[b * capacity : (b + 1) * capacity, :] = rows.astype(jnp.bfloat16)

    rows = rows_ref[...]
    gate = jnp.dot(rows, gate_ref[...], preferred_element_type=jnp.float32)
    up = jnp.dot(rows, up_ref[...], preferred_element_type=jnp.float32)
    hidden = (gate / (1.0 + jnp.exp(-gate)) * up).astype(jnp.bfloat16)
    value = jnp.dot(hidden, down_ref[...], preferred_element_type=jnp.float32)

    @pl.when(step == 0)
    def _():
        acc_ref[...] = value

    @pl.when(step > 0)
    def _():
        acc_ref[...] += value

    @pl.when(step == steps - 1)
    def _():
        for b in range(blocks):
            part = acc_ref[b * capacity : (b + 1) * capacity, :].astype(jnp.bfloat16)
            spread = jnp.dot(pick_ref[b], part, preferred_element_type=jnp.float32)
            outs[b][...] = (spread * weight_ref[b]).astype(jnp.bfloat16)


def run_expert(mask, pieces, w_gate, w_up, w_down, capacity):
    blocks = len(pieces)
    tok = pieces[0].shape[0]
    features, units = w_gate.shape
    tile = min(FF_TILE, units)
    steps = units // tile
    whole = pl.BlockSpec(memory_space=pltpu.VMEM)
    return pl.pallas_call(
        functools.partial(
            expert_kernel, blocks=blocks, features=features, capacity=capacity, steps=steps
        ),
        grid=(steps,),
        in_specs=[whole] * (1 + blocks)
        + [
            pl.BlockSpec((features, tile), lambda i: (0, i)),
            pl.BlockSpec((features, tile), lambda i: (0, i)),
            pl.BlockSpec((tile, features), lambda i: (i, 0)),
        ],
        out_specs=[whole] * blocks,
        out_shape=[jax.ShapeDtypeStruct((tok, features), jnp.bfloat16)] * blocks,
        scratch_shapes=[
            pltpu.VMEM((blocks * capacity, features), jnp.bfloat16),
            pltpu.VMEM((blocks * capacity, features), jnp.float32),
            pltpu.VMEM((blocks, tok, capacity), jnp.bfloat16),
            pltpu.VMEM((blocks, tok, 1), jnp.float32),
        ],
        compiler_params=pltpu.CompilerParams(
            dimension_semantics=("arbitrary",), vmem_limit_bytes=48 * 1024 * 1024
        ),
        name="experts",
    )(mask, *pieces, w_gate, w_up, w_down)


def per_device(tokens, norm_gain, routes, route_weights, w_gate, w_up, w_down, final_gain):
    tok_count, features = tokens.shape
    ep_size = lax.axis_size("ep")
    exp_local = w_gate.shape[0]
    experts_all = exp_local * ep_size
    capacity = max(2, min(tok_count, 2 * tok_count * TOP_K // experts_all))
    capacity = -(-capacity // 16) * 16
    groups = ep_size // 4

    def swap(value, bit):
        return lax.ppermute(value, "ep", [(i, i ^ bit) for i in range(ep_size)])

    tokens_f = tokens.astype(jnp.float32)
    inverse = lax.rsqrt(jnp.mean(tokens_f * tokens_f, axis=1, keepdims=True) + EPS)
    normed = (tokens_f * inverse * norm_gain[None, :]).astype(jnp.bfloat16)
    chosen = routes[:, :, None] == jnp.arange(experts_all, dtype=jnp.int32)[None, None, :]
    table = jnp.sum(jnp.where(chosen, route_weights[:, :, None], 0.0), axis=1)
    high = lax.reduce_precision(table, 8, 7)
    side = jnp.concatenate([high, table - high], axis=1).astype(jnp.bfloat16)
    side = jnp.pad(side, ((0, 0), (0, -side.shape[1] % LANES)))
    own = jnp.concatenate([normed, side], axis=1)
    column = [own]
    for d in range(1, groups):
        column.append(swap(column[d & (d - 1)], 4 * (d & -d)))
    pieces = []
    for d in range(groups):
        across = swap(column[d], 2)
        pieces.append([column[d], across, swap(column[d], 1), swap(across, 1)])
    lanes = jnp.arange(side.shape[1], dtype=jnp.int32)[None, :]
    half = max(1, groups // 2)
    sums = [None] * groups
    for start in range(0, groups, half):
        parts = range(start, min(groups, start + half))
        flat = [piece for d in parts for piece in pieces[d]]
        outs = None
        for e in range(exp_local):
            mine = lax.axis_index("ep") * exp_local + e
            mask = ((lanes == mine) | (lanes == experts_all + mine)).astype(jnp.float32)
            mask = jnp.broadcast_to(mask, (8, side.shape[1]))
            found = run_expert(mask, flat, w_gate[e], w_up[e], w_down[e], capacity)
            outs = found if outs is None else [a + b for a, b in zip(outs, found)]
        for n, d in enumerate(parts):
            sums[d] = outs[4 * n : 4 * n + 4]

    def join(a, b):
        return (a.astype(jnp.float32) + b.astype(jnp.float32)).astype(jnp.bfloat16)

    for d in reversed(range(groups)):
        near, across, near_other, across_other = sums[d]
        across = join(across, swap(across_other, 1))
        near = join(near, swap(near_other, 1))
        sums[d] = near.astype(jnp.float32) + swap(across, 2).astype(jnp.float32)
    for d in reversed(range(1, groups)):
        came = swap(sums[d].astype(jnp.bfloat16), 4 * (d & -d))
        sums[d & (d - 1)] = sums[d & (d - 1)] + came.astype(jnp.float32)
    if lax.axis_size("tp") > 1:
        sums[0] = lax.psum_scatter(sums[0], "tp", scatter_dimension=1, tiled=True)
    combined = sums[0]
    squares_all = lax.psum(jnp.sum(combined * combined, axis=1), "tp")
    inverse_out = lax.rsqrt(squares_all / features + EPS)
    return (combined * inverse_out[:, None] * final_gain[None, :]).astype(jnp.bfloat16)


def solution(mesh):
    placed = (
        P(("grp", "ep"), None),
        P(),
        P(("grp", "ep"), None),
        P(("grp", "ep"), None),
        P("ep", None, "tp"),
        P("ep", None, "tp"),
        P("ep", "tp", None),
        P("tp"),
    )
    return jax.shard_map(
        per_device, mesh=mesh, in_specs=placed, out_specs=P(("grp", "ep"), "tp"), check_vma=False
    )
```

```python
import functools

import jax
import jax.numpy as jnp
from jax import lax
from jax.experimental import pallas as pl
from jax.experimental.pallas import tpu as pltpu
from jax.sharding import PartitionSpec as P


TOP_K = 6
EPS = 1e-06
LANES = 128
TILE = 512
VMEM_MIB = 48


def expert_kernel(*refs, blocks, features, capacity, first, second):
    mask_ref, *refs = refs
    pieces, refs = refs[:blocks], refs[blocks:]
    gate_ref, up_ref, down_ref, *refs = refs
    outs, refs = refs[:blocks], refs[blocks:]
    rows_ref, hidden_ref, pick_ref, weight_ref = refs
    tok = pieces[0].shape[0]
    units = hidden_ref.shape[1]
    tile = units // first
    width = features // second

    def dispatch():
        later = lax.broadcasted_iota(jnp.int32, (tok, tok), 0)
        earlier = lax.broadcasted_iota(jnp.int32, (tok, tok), 1)
        below = (earlier < later).astype(jnp.bfloat16)
        slots = lax.broadcasted_iota(jnp.int32, (tok, capacity), 1).astype(jnp.float32)
        for b in range(blocks):
            side = pieces[b][:, features:].astype(jnp.float32)
            weight = jnp.sum(side * mask_ref[0:1, :], axis=1, keepdims=True)
            used = weight > 0
            flags = jnp.broadcast_to(used.astype(jnp.float32), (tok, LANES)).astype(jnp.bfloat16)
            place = jnp.dot(below, flags, preferred_element_type=jnp.float32)[:, :capacity]
            pick = ((place == slots) & used).astype(jnp.bfloat16)
            pick_ref[b] = pick
            weight_ref[b] = weight
            rows = lax.dot_general(
                pick,
                pieces[b][:, :features],
                (((0,), (0,)), ((), ())),
                preferred_element_type=jnp.float32,
            )
            rows_ref[b * capacity : (b + 1) * capacity, :] = rows.astype(jnp.bfloat16)

    def widen(gate_w, up_w, at):
        rows = rows_ref[...]
        gate = jnp.dot(rows, gate_w, preferred_element_type=jnp.float32)
        up = jnp.dot(rows, up_w, preferred_element_type=jnp.float32)
        hidden_ref[:, pl.ds(at, tile)] = (gate / (1.0 + jnp.exp(-gate)) * up).astype(jnp.bfloat16)

    def narrow(down_w, at):
        value = jnp.dot(hidden_ref[...], down_w, preferred_element_type=jnp.float32)
        value = value.astype(jnp.bfloat16)
        for b in range(blocks):
            part = value[b * capacity : (b + 1) * capacity, :]
            spread = jnp.dot(pick_ref[b], part, preferred_element_type=jnp.float32)
            outs[b][:, pl.ds(at, width)] = (spread * weight_ref[b]).astype(jnp.bfloat16)

    step = pl.program_id(0)
    pl.when(step == 0)(dispatch)

    @pl.when(step < first)
    def _():
        widen(gate_ref[...], up_ref[...], pl.multiple_of(step * tile, tile))

    @pl.when(step >= first)
    def _():
        narrow(down_ref[...], pl.multiple_of((step - first) * width, width))


def run_expert(mask, pieces, w_gate, w_up, w_down, capacity):
    blocks = len(pieces)
    tok = pieces[0].shape[0]
    features, units = w_gate.shape
    first = max(1, units // TILE)
    second = max(1, features // TILE)
    tile, width = units // first, features // second
    whole = pl.BlockSpec(memory_space=pltpu.VMEM)
    return pl.pallas_call(
        functools.partial(
            expert_kernel,
            blocks=blocks,
            features=features,
            capacity=capacity,
            first=first,
            second=second,
        ),
        grid=(first + second,),
        in_specs=[whole] * (1 + blocks)
        + [pl.BlockSpec((features, tile), lambda i: (0, jnp.minimum(i, first - 1)))] * 2
        + [pl.BlockSpec((units, width), lambda i: (0, jnp.maximum(i - first, 0)))],
        out_specs=[whole] * blocks,
        out_shape=[jax.ShapeDtypeStruct((tok, features), jnp.bfloat16)] * blocks,
        scratch_shapes=[
            pltpu.VMEM((blocks * capacity, features), jnp.bfloat16),
            pltpu.VMEM((blocks * capacity, units), jnp.bfloat16),
            pltpu.VMEM((blocks, tok, capacity), jnp.bfloat16),
            pltpu.VMEM((blocks, tok, 1), jnp.float32),
        ],
        compiler_params=pltpu.CompilerParams(
            dimension_semantics=("arbitrary",), vmem_limit_bytes=VMEM_MIB * 1024 * 1024
        ),
        name="experts",
    )(mask, *pieces, w_gate, w_up, w_down)


def per_device(tokens, norm_gain, routes, route_weights, w_gate, w_up, w_down, final_gain):
    tok_count, features = tokens.shape
    ep_size = lax.axis_size("ep")
    exp_local = w_gate.shape[0]
    experts_all = exp_local * ep_size
    capacity = max(2, min(tok_count, 2 * tok_count * TOP_K // experts_all))
    capacity = -(-capacity // 16) * 16
    groups = ep_size // 4

    def swap(value, bit):
        return lax.ppermute(value, "ep", [(i, i ^ bit) for i in range(ep_size)])

    def join(a, b):
        return a.astype(jnp.float32) + b.astype(jnp.float32)

    tokens_f = tokens.astype(jnp.float32)
    inverse = lax.rsqrt(jnp.mean(tokens_f * tokens_f, axis=1, keepdims=True) + EPS)
    normed = (tokens_f * inverse * norm_gain[None, :]).astype(jnp.bfloat16)
    chosen = routes[:, :, None] == jnp.arange(experts_all, dtype=jnp.int32)[None, None, :]
    table = jnp.sum(jnp.where(chosen, route_weights[:, :, None], 0.0), axis=1)
    high = lax.reduce_precision(table, 8, 7)
    side = jnp.concatenate([high, table - high], axis=1).astype(jnp.bfloat16)
    side = jnp.pad(side, ((0, 0), (0, -side.shape[1] % LANES)))
    own = jnp.concatenate([normed, side], axis=1)
    column = [own]
    for d in range(1, groups):
        column.append(swap(column[d & (d - 1)], 4 * (d & -d)))
    pieces = []
    for d in range(groups):
        across = swap(column[d], 2)
        pieces.append([column[d], across, swap(column[d], 1), swap(across, 1)])
    lanes = jnp.arange(side.shape[1], dtype=jnp.int32)[None, :]
    half = max(1, groups // 2)
    plan = [tuple(range(half)), tuple(range(half, groups))]
    sums = [None] * groups
    gone = []
    for parts in plan:
        flat = [piece for d in parts for piece in pieces[d]]
        outs = None
        for e in range(exp_local):
            mine = lax.axis_index("ep") * exp_local + e
            mask = ((lanes == mine) | (lanes == experts_all + mine)).astype(jnp.float32)
            mask = jnp.broadcast_to(mask, (8, side.shape[1]))
            if gone and e == 0:
                mask, *kept = lax.optimization_barrier((mask, *(sums[d][1] for d in gone)))
                for d, value in zip(gone, kept):
                    sums[d] = (sums[d][0], value)
            found = run_expert(mask, flat, w_gate[e], w_up[e], w_down[e], capacity)
            outs = found if outs is None else [a + b for a, b in zip(outs, found)]
        gone = list(reversed(parts))
        for d in gone:
            n = 4 * (d - parts[0])
            near, across, near_other, across_other = outs[n : n + 4]
            across = join(across, swap(across_other, 1)).astype(jnp.bfloat16)
            sums[d] = ((near, near_other), across)
    for d in reversed(range(groups)):
        (near, near_other), across = sums[d]
        came = swap(across, 2)
        sums[d] = join(near, swap(near_other, 1)) + came.astype(jnp.float32)
    for d in reversed(range(1, groups)):
        came = swap(sums[d].astype(jnp.bfloat16), 4 * (d & -d))
        sums[d & (d - 1)] = sums[d & (d - 1)] + came.astype(jnp.float32)
    if lax.axis_size("tp") > 1:
        sums[0] = lax.psum_scatter(sums[0], "tp", scatter_dimension=1, tiled=True)
    combined = sums[0]
    squares_all = lax.psum(jnp.sum(combined * combined, axis=1), "tp")
    inverse_out = lax.rsqrt(squares_all / features + EPS)
    return (combined * inverse_out[:, None] * final_gain[None, :]).astype(jnp.bfloat16)


def solution(mesh):
    placed = (
        P(("grp", "ep"), None),
        P(),
        P(("grp", "ep"), None),
        P(("grp", "ep"), None),
        P("ep", None, "tp"),
        P("ep", None, "tp"),
        P("ep", "tp", None),
        P("tp"),
    )

    return jax.shard_map(
        per_device, mesh=mesh, in_specs=placed, out_specs=P(("grp", "ep"), "tp"), check_vma=False
    )
```
